32 devices in a mesh: sp: 4 (over z), tp: 8 (over y, x, core).
Axes of the slice: x: 2, y: 2, z: 4, core: 2. Of those that a mesh axis runs over, the one named last changes fastest.
Arguments:
- target: bfloat16 [512, 2048], P('sp'), may hold values from -6 to 6
- source: bfloat16 [1024, 2048], P(('sp', 'tp')), may hold values from -6 to 6
- cotangent: bfloat16 [512, 2048], P('sp'), may hold values from -6 to 6
- target_gain: float32 [2048], replicated, may hold values from 0.1 to 1.9
- source_gain: float32 [2048], replicated, may hold values from 0.1 to 1.9
- query_weight: bfloat16 [2048, 8192], P(None, 'tp'), may hold values from -4 to 4
- key_weight: bfloat16 [2048, 2048], P(None, 'tp'), may hold values from -1 to 1
- value_projection_weight: bfloat16 [2048, 2048], P(None, 'tp'), may hold values from -0.125 to 0.125
- output_weight: bfloat16 [8192, 2048], P('tp'), may hold values from -0.0625 to 0.0625
Outputs:
- target_grad: float32 [512, 2048], P(('sp', 'tp'))
- source_grad: float32 [1024, 2048], P(('sp', 'tp'))
- key_weight_grad: float32 [2048, 2048], P(None, 'tp')
The draws below stay inside these ranges and needn't reach their ends.
All inputs are finite; a program needn't handle non-finite values.
Results may differ from the reference program's by a relative error of at most 0.018.
The reference program's roundings to bfloat16 on the way count: a program that leaves them out, or rounds other values in their place, can miss the bound.
Values may be sent and summed in bfloat16 or wider, within the bound.
A program may use at most 64 MiB of HBM per device.

```python
import jax
import jax.numpy as jnp
from jax import lax

MODEL_WIDTH = 2048
QUERY_HEADS = 32
KEY_VALUE_HEADS = 8
HEAD_SIZE = 256
TGT = 512
SOURCE_TOTAL = 1024


def drawn_rows(key):
    folded = jax.random.fold_in(key, 11)
    target_key, source_key = jax.random.split(folded, 2)
    source_rows = jax.random.normal(source_key, (SOURCE_TOTAL, MODEL_WIDTH), jnp.float32)
    target_rows = jax.random.normal(target_key, (TGT, MODEL_WIDTH), jnp.float32)
    return (jnp.clip(target_rows, -6.0, 6.0), jnp.clip(source_rows, -6.0, 6.0))


def paired_weights(key):
    folded = jax.random.fold_in(key, 23)
    key_portion, query_part = jax.random.split(folded, 2)
    key_projection_matrix = jnp.clip(jax.random.normal(key_portion, (MODEL_WIDTH, KEY_VALUE_HEADS * HEAD_SIZE), jnp.float32) * MODEL_WIDTH ** (-0.5), -1.0, 1.0)
    query_matrix = jax.random.normal(query_part, (MODEL_WIDTH, QUERY_HEADS * HEAD_SIZE), jnp.float32) * MODEL_WIDTH ** (-0.5)
    return (jnp.clip(query_matrix, -4.0, 4.0), key_projection_matrix)


def draw_target(key, part):
    return drawn_rows(key)[0].astype(jnp.bfloat16)


def draw_source(key, part):
    return drawn_rows(key)[1].astype(jnp.bfloat16)


def draw_query_weight(key, part):
    return paired_weights(key)[0].astype(jnp.bfloat16)


def draw_key_weight(key, part):
    return paired_weights(key)[1].astype(jnp.bfloat16)


def level_of(stream_key, shape, pieces, smallest, largest):
    level = 1.0
    for position, parts in pieces:
        steps = jax.random.uniform(jax.random.fold_in(jax.random.fold_in(stream_key, 6), position), (parts,), jnp.float32, smallest / len(pieces), largest / len(pieces))
        level = level * jnp.repeat(jnp.exp(steps), shape[position] // parts).reshape((-1,) + (1,) * (len(shape) - 1 - position))
    return level


def gaussian(key, extent, deviation, bound, pieces=(), kind=jnp.bfloat16):
    drawn = deviation * jax.random.normal(key, extent, jnp.float32)
    if pieces:
        drawn = drawn * level_of(key, extent, pieces, -0.22, 0.18)
    return jnp.clip(drawn, -bound, bound).astype(kind)


def setup_inputs(seed: int = 0) -> dict:
    key_list = jax.random.split(jax.random.key(seed), 10)
    target = draw_target(jax.random.fold_in(key_list[9], 71), 0)
    source = draw_source(jax.random.fold_in(key_list[9], 71), 0)
    cotangent = gaussian(key_list[2], (TGT, MODEL_WIDTH), 1.0, 6.0, ((0, 4),))
    target_gain = jnp.clip(1.0 + 0.18 * jax.random.normal(key_list[3], (MODEL_WIDTH,), jnp.float32), 0.1, 1.9)
    source_gain = jnp.clip(1.0 + 0.18 * jax.random.normal(key_list[4], (MODEL_WIDTH,), jnp.float32), 0.1, 1.9)
    query_weight = draw_query_weight(jax.random.fold_in(key_list[9], 71), 0)
    key_weight = draw_key_weight(jax.random.fold_in(key_list[9], 71), 0)
    value_projection_weight = gaussian(key_list[7], (MODEL_WIDTH, KEY_VALUE_HEADS * HEAD_SIZE), MODEL_WIDTH ** -0.5, 0.125, ((1, 8),))
    output_weight = gaussian(key_list[8], (QUERY_HEADS * HEAD_SIZE, MODEL_WIDTH), (QUERY_HEADS * HEAD_SIZE) ** -0.5, 0.0625, ((0, 8),))
    return {"target": target, "source": source, "cotangent": cotangent, "target_gain": target_gain, "source_gain": source_gain, "query_weight": query_weight, "key_weight": key_weight, "value_projection_weight": value_projection_weight, "output_weight": output_weight}


EPSILON = 1e-05

def norm_rows(rows):
    values = rows.astype(jnp.float32)
    centred = values - lax.optimization_barrier(jnp.mean(values, axis=-1, keepdims=True))
    inverse = lax.rsqrt(lax.optimization_barrier(jnp.mean(centred * centred, axis=-1, keepdims=True)) + EPSILON)
    return (centred * inverse, inverse)

def norm_back(scaled, inverse, gain, upstream):
    weighted = upstream * gain
    spread = lax.optimization_barrier(jnp.mean(weighted * scaled, axis=-1, keepdims=True))
    return inverse * (weighted - lax.optimization_barrier(jnp.mean(weighted, axis=-1, keepdims=True)) - scaled * spread)

def reference(target, source, cotangent, target_gain, source_gain, query_weight, key_weight, value_projection_weight, output_weight):
    tgt_scaled, tgt_inverse = norm_rows(target)
    tgt_normed = (tgt_scaled * target_gain).astype(jnp.bfloat16)
    src_scaled, src_inverse = norm_rows(source)
    src_normed = (src_scaled * source_gain).astype(jnp.bfloat16)
    queries = jnp.dot(tgt_normed, query_weight, preferred_element_type=jnp.float32).astype(jnp.bfloat16)
    key_rows = jnp.dot(src_normed, key_weight, preferred_element_type=jnp.float32).astype(jnp.bfloat16)
    value_rows = jnp.dot(src_normed, value_projection_weight, preferred_element_type=jnp.float32).astype(jnp.bfloat16)
    out_grads = jnp.dot(cotangent, output_weight.T, preferred_element_type=jnp.float32).astype(jnp.bfloat16)
    heads_per_group = QUERY_HEADS // KEY_VALUE_HEADS
    score_scale = HEAD_SIZE ** (-0.5)

    def one_head(head_index):
        kv_index = head_index // heads_per_group
        query_head = lax.dynamic_slice_in_dim(queries, head_index * HEAD_SIZE, HEAD_SIZE, 1)
        grad_head = lax.dynamic_slice_in_dim(out_grads, head_index * HEAD_SIZE, HEAD_SIZE, 1)
        key_head = lax.dynamic_slice_in_dim(key_rows, kv_index * HEAD_SIZE, HEAD_SIZE, 1)
        value_head = lax.dynamic_slice_in_dim(value_rows, kv_index * HEAD_SIZE, HEAD_SIZE, 1)
        scores = jnp.dot(query_head, key_head.T, preferred_element_type=jnp.float32) * score_scale
        highest = lax.optimization_barrier(jnp.max(scores, axis=1, keepdims=True))
        weights = jnp.exp(scores - highest)
        totals = lax.optimization_barrier(jnp.sum(weights, axis=1, keepdims=True))
        products = jnp.dot(grad_head, value_head.T, preferred_element_type=jnp.float32)
        drifts = lax.optimization_barrier(jnp.sum(weights * products, axis=1, keepdims=True)) / totals
        softmax_weights = jnp.exp(scores - (highest + jnp.log(totals)))
        slopes = (softmax_weights * (products - drifts) * score_scale).astype(jnp.bfloat16)
        attention = softmax_weights.astype(jnp.bfloat16)
        query_grad = jnp.dot(slopes, key_head, preferred_element_type=jnp.float32)
        key_grad = jnp.dot(slopes.T, query_head, preferred_element_type=jnp.float32)
        value_grad = jnp.dot(attention.T, grad_head, preferred_element_type=jnp.float32)
        return (query_grad, key_grad, value_grad)
    query_grads, key_gradient_rows, value_gradient_rows = lax.map(one_head, jnp.arange(QUERY_HEADS, dtype=jnp.int32))
    query_flat = jnp.transpose(query_grads, (1, 0, 2)).reshape(TGT, QUERY_HEADS * HEAD_SIZE).astype(jnp.bfloat16)
    key_running_sums = lax.optimization_barrier(jnp.sum(key_gradient_rows.reshape(KEY_VALUE_HEADS, heads_per_group, SOURCE_TOTAL, HEAD_SIZE), axis=1))
    value_running_sums = lax.optimization_barrier(jnp.sum(value_gradient_rows.reshape(KEY_VALUE_HEADS, heads_per_group, SOURCE_TOTAL, HEAD_SIZE), axis=1))
    key_flattened = jnp.transpose(key_running_sums, (1, 0, 2)).reshape(SOURCE_TOTAL, KEY_VALUE_HEADS * HEAD_SIZE).astype(jnp.bfloat16)
    value_flattened = jnp.transpose(value_running_sums, (1, 0, 2)).reshape(SOURCE_TOTAL, KEY_VALUE_HEADS * HEAD_SIZE).astype(jnp.bfloat16)
    source_upstream = jnp.dot(key_flattened, key_weight.T, preferred_element_type=jnp.float32) + jnp.dot(value_flattened, value_projection_weight.T, preferred_element_type=jnp.float32)
    source_grad = norm_back(src_scaled, src_inverse, source_gain, source_upstream)
    target_upstream = jnp.dot(query_flat, query_weight.T, preferred_element_type=jnp.float32)
    target_grad = cotangent.astype(jnp.float32) + norm_back(tgt_scaled, tgt_inverse, target_gain, target_upstream)
    key_weight_grad = jnp.dot(src_normed.T, key_flattened, preferred_element_type=jnp.float32)
    return (target_grad, source_grad, key_weight_grad)
```

```python
import functools

import jax
import jax.numpy as jnp
from jax import lax
from jax.experimental import pallas as pl
from jax.experimental.pallas import tpu as pltpu
from jax.sharding import PartitionSpec as P

HEAD_SIZE = 256


EPSILON = 1e-05


def as_sent(array):

    def short(part):
        return part.astype(jnp.bfloat16) if part.dtype == jnp.float32 else part

    return jax.tree.map(short, array)


def partner_2(value, axis, bit):
    mask = 2**bit
    pairs = [(source, source ^ mask) for source in range(lax.axis_size(axis))]
    return lax.ppermute(value, axis, pairs)


def combined_all(value, axis, join):
    pieces = jax.tree.map(lambda part: lax.all_gather(part, axis), value)
    head = jax.tree.map(lambda part: part[0], pieces)
    tail = jax.tree.map(lambda part: part[1:], pieces)
    running, _ = lax.scan(lambda running, piece: (join(running, piece), None), head, tail)
    return running


def norm_rows(rows):
    values = rows.astype(jnp.float32)
    centred = values - jnp.mean(values, axis=-1, keepdims=True)
    inverse = lax.rsqrt(jnp.mean(centred * centred, axis=-1, keepdims=True) + EPSILON)
    return (centred * inverse, inverse)


def norm_back(scaled, inverse, gain, upstream):
    weighted = upstream * gain
    spread = jnp.mean(weighted * scaled, axis=-1, keepdims=True)
    return inverse * (weighted - jnp.mean(weighted, axis=-1, keepdims=True) - scaled * spread)


def times_transposed(left, right):
    return lax.dot_general(
        left, right, (((1,), (1,)), ((), ())), preferred_element_type=jnp.float32
    )


def split_heads(flat):
    return flat.reshape(flat.shape[0], flat.shape[1] // HEAD_SIZE, HEAD_SIZE)


def head_scores(queries, key_rows):
    return jnp.einsum(
        "rhd,sd->hrs", queries, key_rows, preferred_element_type=jnp.float32
    ) * HEAD_SIZE ** (-0.5)


def block_statistics(queries, out_grads, key_rows, value_rows):
    scores = head_scores(queries, key_rows)
    highest = jnp.max(scores, axis=2)
    weights = jnp.exp(scores - highest[:, :, None])
    products = jnp.einsum("rhd,sd->hrs", out_grads, value_rows, preferred_element_type=jnp.float32)
    return (highest, jnp.sum(weights, axis=2), jnp.sum(weights * products, axis=2))


def combine_statistics(former, latter):
    highest = jnp.maximum(former[0], latter[0])
    early_scale = jnp.exp(former[0] - highest)
    late_scale = jnp.exp(latter[0] - highest)
    return (
        highest,
        former[1] * early_scale + latter[1] * late_scale,
        former[2] * early_scale + latter[2] * late_scale,
    )


def score_grads(queries, out_grads, key_rows, value_rows, log_total, drifts):
    scores = head_scores(queries, key_rows)
    softmax_weights = jnp.exp(scores - log_total[:, :, None])
    products = jnp.einsum("rhd,sd->hrs", out_grads, value_rows, preferred_element_type=jnp.float32)
    slopes = (softmax_weights * (products - drifts[:, :, None]) * HEAD_SIZE ** (-0.5)).astype(
        jnp.bfloat16
    )
    return (softmax_weights.astype(jnp.bfloat16), slopes)


def join_heads(stacked):
    position = lax.axis_index("tp")
    part_cols = stacked.shape[2]
    bit_level = 0
    while part_cols < HEAD_SIZE:
        partner = jax.tree.map(
            lambda part, own: part.astype(own.dtype),
            partner_2(as_sent(stacked), "tp", bit_level),
            stacked,
        )
        upper_half = position >> bit_level & 1
        stacked = jnp.where(
            upper_half == 0,
            jnp.concatenate((stacked, partner), 2),
            jnp.concatenate((partner, stacked), 2),
        )
        part_cols = part_cols * 2
        bit_level = bit_level + 1
    return stacked


def split_sums(stacked, part_cols):
    position = lax.axis_index("tp")
    bit_count = (HEAD_SIZE // part_cols).bit_length() - 1
    for bit_level in reversed(range(bit_count)):
        half_cols = stacked.shape[2] // 2
        lower_half = stacked[:, :, :half_cols]
        upper_cols = stacked[:, :, half_cols:]
        upper_half = position >> bit_level & 1
        kept_half = jnp.where(upper_half == 0, lower_half, upper_cols)
        sent_half = jnp.where(upper_half == 0, upper_cols, lower_half)
        stacked = kept_half + partner_2(sent_half, "tp", bit_level)
    return stacked


def on_device(
    target,
    source,
    cotangent,
    target_gain,
    source_gain,
    query_weight,
    key_weight,
    value_projection_weight,
    output_weight,
):
    part_cols = key_weight.shape[1]
    src_scaled, src_inverse = norm_rows(source)
    src_normed = (src_scaled * source_gain).astype(jnp.bfloat16)
    tgt_scaled, tgt_inverse = norm_rows(target)
    tgt_normed = (tgt_scaled * target_gain).astype(jnp.bfloat16)
    block_rows = lax.all_gather(src_normed, "tp", axis=0, tiled=True)
    key_portion = jnp.dot(block_rows, key_weight, preferred_element_type=jnp.float32).astype(
        jnp.bfloat16
    )
    value_part = jnp.dot(
        block_rows, value_projection_weight, preferred_element_type=jnp.float32
    ).astype(jnp.bfloat16)
    parted = jnp.stack((key_portion, value_part))
    queries = split_heads(
        jnp.dot(tgt_normed, query_weight, preferred_element_type=jnp.float32).astype(jnp.bfloat16)
    )
    out_grads = split_heads(times_transposed(cotangent, output_weight).astype(jnp.bfloat16))
    head_count = queries.shape[1]
    own_rows = queries.shape[0]
    own_keys = join_heads(parted)
    all_queries, all_grads = (
        lax.all_gather(queries, "sp", axis=0, tiled=True),
        lax.all_gather(out_grads, "sp", axis=0, tiled=True),
    )
    partial_value = block_statistics(all_queries, all_grads, own_keys[0], own_keys[1])
    highest, totals, weighted = combined_all(partial_value, "sp", combine_statistics)
    log_total = highest + jnp.log(totals)
    drifts = weighted / totals
    attention, slopes = score_grads(
        all_queries, all_grads, own_keys[0], own_keys[1], log_total, drifts
    )
    key_gradient_rows = jnp.einsum(
        "hrs,rhd->sd", slopes, all_queries, preferred_element_type=jnp.float32
    )
    value_gradient_rows = jnp.einsum(
        "hrs,rhd->sd", attention, all_grads, preferred_element_type=jnp.float32
    )
    row_start = lax.axis_index("sp") * own_rows
    own_log = lax.dynamic_slice_in_dim(log_total, row_start, own_rows, 1)
    own_drifts = lax.dynamic_slice_in_dim(drifts, row_start, own_rows, 1)
    pieces = lax.all_gather(own_keys, "sp", axis=1, tiled=True)
    unused, slopes = score_grads(queries, out_grads, pieces[0], pieces[1], own_log, own_drifts)
    query_grads = jnp.einsum("hrs,sd->rhd", slopes, pieces[0], preferred_element_type=jnp.float32)
    summed = split_sums(jnp.stack((key_gradient_rows, value_gradient_rows)), part_cols)
    key_flattened = summed[0].astype(jnp.bfloat16)
    value_flattened = summed[1].astype(jnp.bfloat16)
    weight_part = lax.dot_general(
        block_rows, key_flattened, (((0,), (0,)), ((), ())), preferred_element_type=jnp.float32
    )
    key_weight_grad = lax.psum(weight_part.astype(jnp.bfloat16), "sp").astype(jnp.float32)
    source_upstream = lax.psum_scatter(
        (
            times_transposed(key_flattened, key_weight)
            + times_transposed(value_flattened, value_projection_weight)
        ).astype(jnp.bfloat16),
        "tp",
        scatter_dimension=0,
        tiled=True,
    ).astype(jnp.float32)
    source_grad = norm_back(src_scaled, src_inverse, source_gain, source_upstream)
    query_flat = query_grads.astype(jnp.bfloat16).reshape(own_rows, head_count * HEAD_SIZE)
    out_rows = own_rows // lax.axis_size("tp")
    out_start = lax.axis_index("tp") * out_rows
    target_upstream = lax.psum_scatter(
        times_transposed(query_flat, query_weight), "tp", scatter_dimension=0, tiled=True
    )
    slice_scaled = lax.dynamic_slice_in_dim(tgt_scaled, out_start, out_rows, 0)
    slice_inverse = lax.dynamic_slice_in_dim(tgt_inverse, out_start, out_rows, 0)
    slice_cotangent = lax.dynamic_slice_in_dim(cotangent, out_start, out_rows, 0)
    target_grad = slice_cotangent.astype(jnp.float32) + norm_back(
        slice_scaled, slice_inverse, target_gain, target_upstream
    )
    return (target_grad, source_grad, key_weight_grad)


MESH = pl.DeviceIdType.MESH
TILE = 256
BF16 = jnp.bfloat16
F32 = jnp.float32


def aligned(index, size):
    return pl.ds(pl.multiple_of(index * size, size), size)


def whole_step(
    n_sp,
    n_tp,
    target_hbm,
    source_hbm,
    cotangent_hbm,
    target_gain,
    source_gain,
    query_hbm,
    key_hbm,
    value_hbm,
    output_hbm,
    target_grad,
    source_grad,
    key_weight_grad,
    tgt,
    cot,
    qw,
    kw,
    vw,
    ow,
    raw,
    normed,
    turned,
    tgt_normed,
    keys,
    values,
    queries,
    grads,
    slopes_s,
    attention_s,
    query_flat,
    sums,
    leaving,
    arriving,
    key_all,
    value_flat,
    up_t,
    up_t_pair,
    up_t_mid,
    up_t_got,
    up_s,
    up_s_pair,
    up_s_mid,
    up_s_got,
    load_sem,
    gather_sem,
    z_send,
    spread_send,
    forward_send,
    sums_send,
    sums_recv,
    key_send,
    key_recv,
    pair_send,
    pair_recv,
    mid_send,
    mid_recv,
):
    z = lax.axis_index("sp")
    t = lax.axis_index("tp")
    n_pair = n_tp // 2
    chip = t // 2
    core = t % 2
    partner = chip * 2 + (1 - core)
    depth = tgt.shape[1]
    tgt_rows = tgt.shape[0]
    src_rows = raw.shape[2]
    block = n_tp * src_rows
    out_rows = tgt_rows // n_tp
    heads = qw.shape[1] // HEAD_SIZE
    scale = HEAD_SIZE ** (-0.5)
    tiles = depth // TILE

    def load(index, src, dst):
        return pltpu.make_async_copy(src, dst, load_sem.at[index])

    load_src = load(0, source_hbm, raw.at[z, t])
    load_tgt = load(1, target_hbm, tgt)
    load_qw = load(2, query_hbm, qw)
    load_cot = load(3, cotangent_hbm, cot)
    load_ow = load(4, output_hbm, ow)
    load_kw = load(5, key_hbm, kw)
    load_vw = load(6, value_hbm, vw)
    for each in (load_src, load_tgt, load_qw, load_cot, load_ow, load_kw, load_vw):
        each.start()

    mates = [(z, ((chip + k) % n_pair) * 2 + core) for k in range(1, n_pair)]
    others = [((z + k) % n_sp, t) for k in range(1, n_sp)]
    barrier = pltpu.get_barrier_semaphore()
    for peer in mates + others + [(z, partner)]:
        pl.semaphore_signal(barrier, inc=1, device_id=peer, device_id_type=MESH)
    pl.semaphore_wait(barrier, len(mates) + len(others) + 1)

    def remote(src, dst, send, recv, peer):
        return pltpu.make_async_remote_copy(
            src_ref=src,
            dst_ref=dst,
            send_sem=send,
            recv_sem=recv,
            device_id=peer,
            device_id_type=MESH,
        )

    pending = []

    def send(*args):
        copy = remote(*args)
        copy.start()
        pending.append(copy)

    def row_copy(zb, tb, sem, peer):
        return (raw.at[zb, tb], raw.at[zb, tb], sem, gather_sem.at[zb, tb], peer)

    def arrive(zb, tb):
        remote(*row_copy(zb, tb, z_send.at[0], (z, partner))).wait_recv()

    def spread(step):
        zb = (z + step) % n_sp
        if step:
            arrive(zb, t)
        for k in range(1, n_pair):
            send(*row_copy(zb, t, spread_send.at[step, k], mates[k - 1]))
        send(*row_copy(zb, t, spread_send.at[step, 0], (z, partner)))

    def forward(step):
        zb = (z + step) % n_sp
        for k in range(1, n_pair):
            tb = ((chip + k) % n_pair) * 2 + core
            arrive(zb, tb)
            send(*row_copy(zb, tb, forward_send.at[step, k], (z, partner)))

    def source_block(step):
        zb = (z + step) % n_sp
        for k in range(n_pair):
            arrive(zb, ((chip + k) % n_pair) * 2 + 1 - core)
        gain = source_gain[...]

        def norm_piece(piece, carry):
            scaled, _ = norm_rows(raw[zb, piece])
            normed[zb, aligned(piece, src_rows), :] = (scaled * gain).astype(BF16)
            return carry

        lax.fori_loop(0, n_tp, norm_piece, 0)
        keys[aligned(zb, block), :] = jnp.dot(
            normed[zb], kw[...], preferred_element_type=F32
        ).astype(BF16)
        values[aligned(zb, block), :] = jnp.dot(
            normed[zb], vw[...], preferred_element_type=F32
        ).astype(BF16)

        def turn(j, carry):
            turned[zb, aligned(j, TILE), :] = normed[zb, :, aligned(j, TILE)].T
            return carry

        lax.fori_loop(0, tiles, turn, 0)

    near_first = sorted(range(1, n_sp), key=lambda k: min(k, n_sp - k))
    load_src.wait()
    for k in near_first:
        send(*row_copy(z, t, z_send.at[k], others[k - 1]))
    spread(0)

    load_tgt.wait()
    norm_step = tgt_rows // n_tp

    def norm_target(piece, carry):
        scaled, _ = norm_rows(tgt[aligned(piece, norm_step), :])
        tgt_normed[aligned(piece, norm_step), :] = (scaled * target_gain[...]).astype(BF16)
        return carry

    lax.fori_loop(0, n_tp, norm_target, 0)
    load_qw.wait()

    def query_head(h, carry):
        queries[aligned(h, tgt_rows), :] = jnp.dot(
            tgt_normed[...], qw[:, aligned(h, HEAD_SIZE)], preferred_element_type=F32
        ).astype(BF16)
        return carry

    lax.fori_loop(0, heads, query_head, 0)
    spread(near_first[0])
    forward(0)
    load_cot.wait()
    load_ow.wait()

    def grad_head(h, carry):
        grads[aligned(h, tgt_rows), :] = times_transposed(
            cot[...], ow[aligned(h, HEAD_SIZE), :]
        ).astype(BF16)
        return carry

    lax.fori_loop(0, heads, grad_head, 0)
    for k in near_first[1:]:
        spread(k)
    load_kw.wait()
    load_vw.wait()
    source_block(0)
    for k in near_first:
        forward(k)
        source_block(k)

    def attend(h, carry):
        rows = aligned(h, tgt_rows)
        scores = times_transposed(queries[rows, :], keys[...]) * scale
        highest = jnp.max(scores, axis=1, keepdims=True)
        weights = jnp.exp(scores - highest)
        totals = jnp.sum(weights, axis=1, keepdims=True)
        products = times_transposed(grads[rows, :], values[...])
        drifts = jnp.sum(weights * products, axis=1, keepdims=True) / totals
        weights = weights * (1.0 / totals)
        attention = weights.astype(BF16)
        slopes = (weights * (products - drifts) * scale).astype(BF16)
        for zb in range(n_sp):
            slopes_s[zb, rows, :] = slopes[:, zb * block : (zb + 1) * block]
            attention_s[zb, rows, :] = attention[:, zb * block : (zb + 1) * block]
        query_flat[:, aligned(h, HEAD_SIZE)] = jnp.dot(
            slopes, keys[...], preferred_element_type=F32
        ).astype(BF16)
        return carry

    lax.fori_loop(0, heads, attend, 0)

    def block_sums(zb, carry):
        sums[zb, 0] = jnp.dot(slopes_s[zb].T, queries[...], preferred_element_type=F32)
        sums[zb, 1] = jnp.dot(attention_s[zb].T, grads[...], preferred_element_type=F32)
        return carry

    lax.fori_loop(0, n_sp, block_sums, 0)

    def sums_copy(side, to, part):
        peer = (z + 1 if side == 0 else z - 1, t)
        return remote(
            leaving.at[to, part],
            arriving.at[side, to, part],
            sums_send.at[to, part],
            sums_recv.at[side, to, part],
            peer,
        )

    def has_upstream(side):
        return z > 0 if side == 0 else z < n_sp - 1

    def sums_wait(side, to, part):
        pltpu.make_async_copy(
            arriving.at[side, to, part],
            arriving.at[side, to, part],
            sums_recv.at[side, to, part],
        ).wait()

    def pass_on(side, far, part):
        to = z + far if side == 0 else z - far
        inside = to < n_sp if side == 0 else to >= 0

        @pl.when(inside)
        def _():
            @pl.when(has_upstream(side))
            def _():
                sums_wait(side, to, part)
                leaving[to, part] = (
                    sums[to, part] + arriving[side, to, part].astype(F32)
                ).astype(BF16)

            @pl.when(jnp.logical_not(has_upstream(side)))
            def _():
                leaving[to, part] = sums[to, part].astype(BF16)

            sums_copy(side, to, part).start()

    def start_edges(side):
        far = n_sp - 1

        for part in range(2):
            pass_on(side, far, part)

    start_edges(0)
    start_edges(1)

    def target_up(j, carry):
        tile = times_transposed(query_flat[...], qw[aligned(j, TILE), :]).astype(BF16)
        for to in range(n_tp):
            up_t[to % 2, to // 2, :, aligned(j, TILE)] = tile[
                to * out_rows : (to + 1) * out_rows
            ]
        return carry

    lax.fori_loop(0, tiles, target_up, 0)

    def pair_copy(which, held, got):
        return remote(
            held.at[1 - core], got, pair_send.at[which], pair_recv.at[which], (z, partner)
        )

    def pair_sum(which, held, got, mid, landed):
        pair_copy(which, held, got).wait_recv()
        for k in list(range(1, n_pair)) + [0]:
            to = (chip + k) % n_pair
            mid[to] = (held[core, to].astype(F32) + got[to].astype(F32)).astype(BF16)
            if k:
                send(
                    mid.at[to],
                    landed.at[chip],
                    mid_send.at[which, k],
                    mid_recv.at[which, chip],
                    mates[k - 1],
                )

    def last_sum(which, mid, landed):
        total = mid[chip].astype(F32)
        for k in range(1, n_pair):
            came = (chip + k) % n_pair
            remote(
                mid.at[came],
                landed.at[came],
                mid_send.at[which, k],
                mid_recv.at[which, came],
                mates[k - 1],
            ).wait_recv()
            total = total + landed[came].astype(F32)
        return total

    target_pair = pair_copy(0, up_t, up_t_pair)
    target_pair.start()
    for far in range(n_sp - 2, 0, -1):
        for part in range(2):
            for side in range(2):
                pass_on(side, far, part)
        if far == n_sp - 2:
            pair_sum(0, up_t, up_t_pair, up_t_mid, up_t_got)
    for part in range(2):
        for side in range(2):

            @pl.when(has_upstream(side))
            def _():
                sums_wait(side, z, part)
                sums[z, part] = sums[z, part] + arriving[side, z, part].astype(F32)

        if part == 0:
            key_all[z] = sums[z, 0].astype(BF16)
            for k in near_first:
                send(
                    key_all.at[z],
                    key_all.at[z],
                    key_send.at[k],
                    key_recv.at[z],
                    others[k - 1],
                )
        else:
            value_flat[...] = sums[z, 1].astype(BF16)

    def source_up(j, carry):
        tile = (
            times_transposed(key_all[z], kw[aligned(j, TILE), :])
            + times_transposed(value_flat[...], vw[aligned(j, TILE), :])
        ).astype(BF16)
        for to in range(n_tp):
            up_s[to % 2, to // 2, :, aligned(j, TILE)] = tile[
                to * src_rows : (to + 1) * src_rows
            ]
        return carry

    lax.fori_loop(0, tiles, source_up, 0)
    source_pair = pair_copy(1, up_s, up_s_pair)
    source_pair.start()

    own = pl.ds(pl.multiple_of(t * out_rows, out_rows), out_rows)
    scaled, inverse = norm_rows(tgt[own, :])
    target_grad[...] = cot[own, :].astype(F32) + norm_back(
        scaled, inverse, target_gain[...], last_sum(0, up_t_mid, up_t_got)
    )
    pair_sum(1, up_s, up_s_pair, up_s_mid, up_s_got)

    def weight_part(step):
        zb = (z + step) % n_sp

        def piece(j, carry):
            product = jnp.dot(
                turned[zb, aligned(j, TILE), :], key_all[zb], preferred_element_type=F32
            )
            if step:
                product = product + key_weight_grad[aligned(j, TILE), :]
            key_weight_grad[aligned(j, TILE), :] = product
            return carry

        lax.fori_loop(0, tiles, piece, 0)

    weight_part(0)
    for k in near_first:
        zb = (z + k) % n_sp
        remote(
            key_all.at[zb], key_all.at[zb], key_send.at[k], key_recv.at[zb], others[k - 1]
        ).wait_recv()
        weight_part(k)

    scaled, inverse = norm_rows(raw[z, t])
    source_grad[...] = norm_back(
        scaled, inverse, source_gain[...], last_sum(1, up_s_mid, up_s_got)
    )
    for copy in pending + [target_pair, source_pair]:
        copy.wait_send()
    for far in range(1, n_sp):
        for part in range(2):
            for side in range(2):
                to = z + far if side == 0 else z - far

                @pl.when(to < n_sp if side == 0 else to >= 0)
                def _():
                    sums_copy(side, to, part).wait_send()


def on_device_any(
    n_sp,
    n_tp,
    target,
    source,
    cotangent,
    target_gain,
    source_gain,
    query_weight,
    key_weight,
    value_projection_weight,
    output_weight,
):
    tgt_rows, depth = target.shape
    src_rows = source.shape[0]
    out_rows = tgt_rows // n_tp
    if (
        key_weight.shape[1] != HEAD_SIZE
        or n_sp < 2
        or n_tp < 4
        or n_tp % 2
        or depth % TILE
        or tgt_rows % (16 * n_tp)
        or src_rows % 16
        or (src_rows * n_tp) % 128
    ):
        return on_device(
            target,
            source,
            cotangent,
            target_gain,
            source_gain,
            query_weight,
            key_weight,
            value_projection_weight,
            output_weight,
        )
    n_pair = n_tp // 2
    block = src_rows * n_tp
    query_cols = query_weight.shape[1]
    heads = query_cols // HEAD_SIZE
    hbm = pl.BlockSpec(memory_space=pl.ANY)
    vmem = pl.BlockSpec(memory_space=pltpu.VMEM)
    dma = pltpu.SemaphoreType.DMA

    def room(*shape, kind=BF16):
        return pltpu.VMEM(shape, kind)

    return pl.pallas_call(
        functools.partial(whole_step, n_sp, n_tp),
        out_shape=(
            jax.ShapeDtypeStruct((out_rows, depth), F32),
            jax.ShapeDtypeStruct((src_rows, depth), F32),
            jax.ShapeDtypeStruct((depth, HEAD_SIZE), F32),
        ),
        in_specs=[hbm, hbm, hbm, vmem, vmem, hbm, hbm, hbm, hbm],
        out_specs=(vmem, vmem, vmem),
        scratch_shapes=[
            room(tgt_rows, depth),
            room(tgt_rows, depth),
            room(depth, query_cols),
            room(depth, HEAD_SIZE),
            room(depth, HEAD_SIZE),
            room(query_cols, depth),
            room(n_sp, n_tp, src_rows, depth),
            room(n_sp, block, depth),
            room(n_sp, depth, block),
            room(tgt_rows, depth),
            room(n_sp * block, HEAD_SIZE),
            room(n_sp * block, HEAD_SIZE),
            room(heads * tgt_rows, HEAD_SIZE),
            room(heads * tgt_rows, HEAD_SIZE),
            room(n_sp, heads * tgt_rows, block),
            room(n_sp, heads * tgt_rows, block),
            room(tgt_rows, query_cols),
            room(n_sp, 2, block, HEAD_SIZE, kind=F32),
            room(n_sp, 2, block, HEAD_SIZE),
            room(2, n_sp, 2, block, HEAD_SIZE),
            room(n_sp, block, HEAD_SIZE),
            room(block, HEAD_SIZE),
            room(2, n_pair, out_rows, depth),
            room(n_pair, out_rows, depth),
            room(n_pair, out_rows, depth),
            room(n_pair, out_rows, depth),
            room(2, n_pair, src_rows, depth),
            room(n_pair, src_rows, depth),
            room(n_pair, src_rows, depth),
            room(n_pair, src_rows, depth),
            dma((7,)),
            dma((n_sp, n_tp)),
            dma((n_sp,)),
            dma((n_sp, n_pair)),
            dma((n_sp, n_pair)),
            dma((n_sp, 2)),
            dma((2, n_sp, 2)),
            dma((n_sp,)),
            dma((n_sp,)),
            dma((2,)),
            dma((2,)),
            dma((2, n_pair)),
            dma((2, n_pair)),
        ],
        compiler_params=pltpu.CompilerParams(
            collective_id=0, has_side_effects=True, vmem_limit_bytes=64 * 1024 * 1024 - 65536
        ),
        name="whole_step",
    )(
        target,
        source,
        cotangent,
        target_gain.reshape(1, depth),
        source_gain.reshape(1, depth),
        query_weight,
        key_weight,
        value_projection_weight,
        output_weight,
    )


def solution(mesh):
    return jax.shard_map(
        functools.partial(on_device_any, mesh.shape["sp"], mesh.shape["tp"]),
        mesh=mesh,
        in_specs=(
            P("sp", None),
            P(("sp", "tp"), None),
            P("sp", None),
            P(),
            P(),
            P(None, "tp"),
            P(None, "tp"),
            P(None, "tp"),
            P("tp", None),
        ),
        out_specs=(P(("sp", "tp"), None), P(("sp", "tp"), None), P(None, "tp")),
        check_vma=False,
    )
```

```python
import functools

import jax
import jax.numpy as jnp
from jax import lax
from jax.experimental import pallas as pl
from jax.experimental.pallas import tpu as pltpu
from jax.sharding import PartitionSpec as P

HEAD_SIZE = 256


EPSILON = 1e-05


def as_sent(array):

    def short(part):
        return part.astype(jnp.bfloat16) if part.dtype == jnp.float32 else part

    return jax.tree.map(short, array)


def partner_2(value, axis, bit):
    mask = 2**bit
    pairs = [(source, source ^ mask) for source in range(lax.axis_size(axis))]
    return lax.ppermute(value, axis, pairs)


def combined_all(value, axis, join):
    pieces = jax.tree.map(lambda part: lax.all_gather(part, axis), value)
    head = jax.tree.map(lambda part: part[0], pieces)
    tail = jax.tree.map(lambda part: part[1:], pieces)
    running, _ = lax.scan(lambda running, piece: (join(running, piece), None), head, tail)
    return running


def norm_rows(rows):
    values = rows.astype(jnp.float32)
    centred = values - jnp.mean(values, axis=-1, keepdims=True)
    inverse = lax.rsqrt(jnp.mean(centred * centred, axis=-1, keepdims=True) + EPSILON)
    return (centred * inverse, inverse)


def norm_back(scaled, inverse, gain, upstream):
    weighted = upstream * gain
    spread = jnp.mean(weighted * scaled, axis=-1, keepdims=True)
    return inverse * (weighted - jnp.mean(weighted, axis=-1, keepdims=True) - scaled * spread)


def times_transposed(left, right):
    return lax.dot_general(
        left, right, (((1,), (1,)), ((), ())), preferred_element_type=jnp.float32
    )


def split_heads(flat):
    return flat.reshape(flat.shape[0], flat.shape[1] // HEAD_SIZE, HEAD_SIZE)


def head_scores(queries, key_rows):
    return jnp.einsum(
        "rhd,sd->hrs", queries, key_rows, preferred_element_type=jnp.float32
    ) * HEAD_SIZE ** (-0.5)


def block_statistics(queries, out_grads, key_rows, value_rows):
    scores = head_scores(queries, key_rows)
    highest = jnp.max(scores, axis=2)
    weights = jnp.exp(scores - highest[:, :, None])
    products = jnp.einsum("rhd,sd->hrs", out_grads, value_rows, preferred_element_type=jnp.float32)
    return (highest, jnp.sum(weights, axis=2), jnp.sum(weights * products, axis=2))


def combine_statistics(former, latter):
    highest = jnp.maximum(former[0], latter[0])
    early_scale = jnp.exp(former[0] - highest)
    late_scale = jnp.exp(latter[0] - highest)
    return (
        highest,
        former[1] * early_scale + latter[1] * late_scale,
        former[2] * early_scale + latter[2] * late_scale,
    )


def score_grads(queries, out_grads, key_rows, value_rows, log_total, drifts):
    scores = head_scores(queries, key_rows)
    softmax_weights = jnp.exp(scores - log_total[:, :, None])
    products = jnp.einsum("rhd,sd->hrs", out_grads, value_rows, preferred_element_type=jnp.float32)
    slopes = (softmax_weights * (products - drifts[:, :, None]) * HEAD_SIZE ** (-0.5)).astype(
        jnp.bfloat16
    )
    return (softmax_weights.astype(jnp.bfloat16), slopes)


def join_heads(stacked):
    position = lax.axis_index("tp")
    part_cols = stacked.shape[2]
    bit_level = 0
    while part_cols < HEAD_SIZE:
        partner = jax.tree.map(
            lambda part, own: part.astype(own.dtype),
            partner_2(as_sent(stacked), "tp", bit_level),
            stacked,
        )
        upper_half = position >> bit_level & 1
        stacked = jnp.where(
            upper_half == 0,
            jnp.concatenate((stacked, partner), 2),
            jnp.concatenate((partner, stacked), 2),
        )
        part_cols = part_cols * 2
        bit_level = bit_level + 1
    return stacked


def split_sums(stacked, part_cols):
    position = lax.axis_index("tp")
    bit_count = (HEAD_SIZE // part_cols).bit_length() - 1
    for bit_level in reversed(range(bit_count)):
        half_cols = stacked.shape[2] // 2
        lower_half = stacked[:, :, :half_cols]
        upper_cols = stacked[:, :, half_cols:]
        upper_half = position >> bit_level & 1
        kept_half = jnp.where(upper_half == 0, lower_half, upper_cols)
        sent_half = jnp.where(upper_half == 0, upper_cols, lower_half)
        stacked = kept_half + partner_2(sent_half, "tp", bit_level)
    return stacked


def on_device(
    target,
    source,
    cotangent,
    target_gain,
    source_gain,
    query_weight,
    key_weight,
    value_projection_weight,
    output_weight,
):
    part_cols = key_weight.shape[1]
    src_scaled, src_inverse = norm_rows(source)
    src_normed = (src_scaled * source_gain).astype(jnp.bfloat16)
    tgt_scaled, tgt_inverse = norm_rows(target)
    tgt_normed = (tgt_scaled * target_gain).astype(jnp.bfloat16)
    block_rows = lax.all_gather(src_normed, "tp", axis=0, tiled=True)
    key_portion = jnp.dot(block_rows, key_weight, preferred_element_type=jnp.float32).astype(
        jnp.bfloat16
    )
    value_part = jnp.dot(
        block_rows, value_projection_weight, preferred_element_type=jnp.float32
    ).astype(jnp.bfloat16)
    parted = jnp.stack((key_portion, value_part))
    queries = split_heads(
        jnp.dot(tgt_normed, query_weight, preferred_element_type=jnp.float32).astype(jnp.bfloat16)
    )
    out_grads = split_heads(times_transposed(cotangent, output_weight).astype(jnp.bfloat16))
    head_count = queries.shape[1]
    own_rows = queries.shape[0]
    own_keys = join_heads(parted)
    all_queries, all_grads = (
        lax.all_gather(queries, "sp", axis=0, tiled=True),
        lax.all_gather(out_grads, "sp", axis=0, tiled=True),
    )
    partial_value = block_statistics(all_queries, all_grads, own_keys[0], own_keys[1])
    highest, totals, weighted = combined_all(partial_value, "sp", combine_statistics)
    log_total = highest + jnp.log(totals)
    drifts = weighted / totals
    attention, slopes = score_grads(
        all_queries, all_grads, own_keys[0], own_keys[1], log_total, drifts
    )
    key_gradient_rows = jnp.einsum(
        "hrs,rhd->sd", slopes, all_queries, preferred_element_type=jnp.float32
    )
    value_gradient_rows = jnp.einsum(
        "hrs,rhd->sd", attention, all_grads, preferred_element_type=jnp.float32
    )
    row_start = lax.axis_index("sp") * own_rows
    own_log = lax.dynamic_slice_in_dim(log_total, row_start, own_rows, 1)
    own_drifts = lax.dynamic_slice_in_dim(drifts, row_start, own_rows, 1)
    pieces = lax.all_gather(own_keys, "sp", axis=1, tiled=True)
    unused, slopes = score_grads(queries, out_grads, pieces[0], pieces[1], own_log, own_drifts)
    query_grads = jnp.einsum("hrs,sd->rhd", slopes, pieces[0], preferred_element_type=jnp.float32)
    summed = split_sums(jnp.stack((key_gradient_rows, value_gradient_rows)), part_cols)
    key_flattened = summed[0].astype(jnp.bfloat16)
    value_flattened = summed[1].astype(jnp.bfloat16)
    weight_part = lax.dot_general(
        block_rows, key_flattened, (((0,), (0,)), ((), ())), preferred_element_type=jnp.float32
    )
    key_weight_grad = lax.psum(weight_part.astype(jnp.bfloat16), "sp").astype(jnp.float32)
    source_upstream = lax.psum_scatter(
        (
            times_transposed(key_flattened, key_weight)
            + times_transposed(value_flattened, value_projection_weight)
        ).astype(jnp.bfloat16),
        "tp",
        scatter_dimension=0,
        tiled=True,
    ).astype(jnp.float32)
    source_grad = norm_back(src_scaled, src_inverse, source_gain, source_upstream)
    query_flat = query_grads.astype(jnp.bfloat16).reshape(own_rows, head_count * HEAD_SIZE)
    out_rows = own_rows // lax.axis_size("tp")
    out_start = lax.axis_index("tp") * out_rows
    target_upstream = lax.psum_scatter(
        times_transposed(query_flat, query_weight), "tp", scatter_dimension=0, tiled=True
    )
    slice_scaled = lax.dynamic_slice_in_dim(tgt_scaled, out_start, out_rows, 0)
    slice_inverse = lax.dynamic_slice_in_dim(tgt_inverse, out_start, out_rows, 0)
    slice_cotangent = lax.dynamic_slice_in_dim(cotangent, out_start, out_rows, 0)
    target_grad = slice_cotangent.astype(jnp.float32) + norm_back(
        slice_scaled, slice_inverse, target_gain, target_upstream
    )
    return (target_grad, source_grad, key_weight_grad)


MESH = pl.DeviceIdType.MESH
TILE = 256
BF16 = jnp.bfloat16
F32 = jnp.float32


def aligned(index, size):
    return pl.ds(pl.multiple_of(index * size, size), size)


def whole_step(
    n_sp,
    n_tp,
    target_hbm,
    source_hbm,
    cotangent_hbm,
    target_gain,
    source_gain,
    query_hbm,
    key_hbm,
    value_hbm,
    output_hbm,
    target_grad,
    source_grad,
    key_weight_grad,
    tgt,
    cot,
    qw,
    kw,
    vw,
    ow,
    raw,
    normed,
    turned,
    tgt_normed,
    keys,
    values,
    queries,
    grads,
    slopes_s,
    attention_s,
    query_flat,
    sums,
    leaving,
    arriving,
    key_all,
    value_flat,
    up_t,
    up_t_pair,
    up_t_mid,
    up_t_got,
    up_s,
    up_s_pair,
    up_s_mid,
    up_s_got,
    load_sem,
    gather_sem,
    z_send,
    spread_send,
    forward_send,
    half_send,
    half_recv,
    sums_send,
    sums_recv,
    key_send,
    key_recv,
    pair_send,
    pair_recv,
    mid_send,
    mid_recv,
):
    z = lax.axis_index("sp")
    t = lax.axis_index("tp")
    n_pair = n_tp // 2
    chip = t // 2
    core = t % 2
    partner = chip * 2 + (1 - core)
    depth = tgt.shape[1]
    tgt_rows = tgt.shape[0]
    src_rows = raw.shape[2]
    block = n_tp * src_rows
    out_rows = tgt_rows // n_tp
    heads = qw.shape[1] // HEAD_SIZE
    scale = HEAD_SIZE ** (-0.5)
    tiles = depth // TILE

    def load(index, src, dst):
        return pltpu.make_async_copy(src, dst, load_sem.at[index])

    load_src = load(0, source_hbm, raw.at[z, t])
    load_tgt = load(1, target_hbm, tgt)
    load_qw = load(2, query_hbm, qw)
    load_cot = load(3, cotangent_hbm, cot)
    load_ow = load(4, output_hbm, ow)
    load_kw = load(5, key_hbm, kw)
    load_vw = load(6, value_hbm, vw)
    for each in (load_src, load_tgt, load_qw, load_cot, load_ow, load_kw, load_vw):
        each.start()

    square = n_pair == 4
    if square:
        across = [chip + 1 - 2 * (chip % 2), (chip + 2) % 4, 3 - chip]
    else:
        across = [(chip + k) % n_pair for k in range(1, n_pair)]
    mates = [(z, other * 2 + core) for other in across]
    others = [((z + k) % n_sp, t) for k in range(1, n_sp)]
    barrier = pltpu.get_barrier_semaphore()
    for peer in mates + others + [(z, partner)]:
        pl.semaphore_signal(barrier, inc=1, device_id=peer, device_id_type=MESH)
    pl.semaphore_wait(barrier, len(mates) + len(others) + 1)

    def remote(src, dst, send, recv, peer):
        return pltpu.make_async_remote_copy(
            src_ref=src,
            dst_ref=dst,
            send_sem=send,
            recv_sem=recv,
            device_id=peer,
            device_id_type=MESH,
        )

    pending = []

    def send(*args):
        copy = remote(*args)
        copy.start()
        pending.append(copy)

    def row_copy(zb, tb, sem, peer):
        return (raw.at[zb, tb], raw.at[zb, tb], sem, gather_sem.at[zb, tb], peer)

    def arrive(zb, tb):
        remote(*row_copy(zb, tb, z_send.at[0], (z, partner))).wait_recv()

    def spread(step):
        zb = (z + step) % n_sp
        if step:
            arrive(zb, t)
        for k in range(1, n_pair):
            if not square or k != 3:
                send(*row_copy(zb, t, spread_send.at[step, k], mates[k - 1]))
        send(*row_copy(zb, t, spread_send.at[step, 0], (z, partner)))

    def forward(step):
        zb = (z + step) % n_sp
        for k in range(1, n_pair):
            tb = mates[k - 1][1]
            if square and k == 3:
                continue
            arrive(zb, tb)
            if square:
                send(*half_copy(zb, tb, k - 1, half_send.at[step, k - 1], mates[2 - k]))
            send(*row_copy(zb, tb, forward_send.at[step, k], (z, partner)))

    def half_copy(zb, tb, half, sem, peer):
        part = raw.at[zb, tb, pl.ds(half * (src_rows // 2), src_rows // 2)]
        return (part, part, sem, half_recv.at[zb, half], peer)

    def far_corner(step):
        if not square:
            return
        zb = (z + step) % n_sp
        tb = mates[2][1]
        for half in range(2):
            remote(*half_copy(zb, tb, half, half_send.at[step, half], mates[0])).wait_recv()
        send(*row_copy(zb, tb, forward_send.at[step, 3], (z, partner)))

    def source_block(step):
        zb = (z + step) % n_sp
        for other in [chip] + across:
            arrive(zb, other * 2 + 1 - core)
        gain = source_gain[...]

        def norm_piece(piece, carry):
            scaled, _ = norm_rows(raw[zb, piece])
            normed[zb, aligned(piece, src_rows), :] = (scaled * gain).astype(BF16)
            return carry

        lax.fori_loop(0, n_tp, norm_piece, 0)
        keys[aligned(zb, block), :] = jnp.dot(
            normed[zb], kw[...], preferred_element_type=F32
        ).astype(BF16)
        values[aligned(zb, block), :] = jnp.dot(
            normed[zb], vw[...], preferred_element_type=F32
        ).astype(BF16)

        def turn(j, carry):
            turned[zb, aligned(j, TILE), :] = normed[zb, :, aligned(j, TILE)].T
            return carry

        lax.fori_loop(0, tiles, turn, 0)

    near_first = sorted(range(1, n_sp), key=lambda k: min(k, n_sp - k))
    load_src.wait()
    for k in near_first:
        send(*row_copy(z, t, z_send.at[k], others[k - 1]))
    spread(0)

    load_tgt.wait()
    norm_step = tgt_rows // n_tp

    def norm_target(piece, carry):
        scaled, _ = norm_rows(tgt[aligned(piece, norm_step), :])
        tgt_normed[aligned(piece, norm_step), :] = (scaled * target_gain[...]).astype(BF16)
        return carry

    lax.fori_loop(0, n_tp, norm_target, 0)
    load_qw.wait()

    def query_head(h, carry):
        queries[aligned(h, tgt_rows), :] = jnp.dot(
            tgt_normed[...], qw[:, aligned(h, HEAD_SIZE)], preferred_element_type=F32
        ).astype(BF16)
        return carry

    lax.fori_loop(0, heads, query_head, 0)
    forward(0)
    spread(near_first[0])
    load_cot.wait()
    load_ow.wait()

    def grad_head(h, carry):
        grads[aligned(h, tgt_rows), :] = times_transposed(
            cot[...], ow[aligned(h, HEAD_SIZE), :]
        ).astype(BF16)
        return carry

    lax.fori_loop(0, heads, grad_head, 0)
    for k in near_first[1:]:
        spread(k)
    load_kw.wait()
    load_vw.wait()
    far_corner(0)
    steps = [0] + near_first
    forward(steps[1])
    for place, k in enumerate(steps):
        source_block(k)
        if place + 1 < n_sp:
            far_corner(steps[place + 1])
        if place + 2 < n_sp:
            forward(steps[place + 2])

    def attend(h, carry):
        rows = aligned(h, tgt_rows)
        scores = times_transposed(queries[rows, :], keys[...]) * scale
        highest = jnp.max(scores, axis=1, keepdims=True)
        weights = jnp.exp(scores - highest)
        totals = jnp.sum(weights, axis=1, keepdims=True)
        products = times_transposed(grads[rows, :], values[...])
        drifts = jnp.sum(weights * products, axis=1, keepdims=True) / totals
        weights = weights * (1.0 / totals)
        attention = weights.astype(BF16)
        slopes = (weights * (products - drifts) * scale).astype(BF16)
        for zb in range(n_sp):
            slopes_s[zb, rows, :] = slopes[:, zb * block : (zb + 1) * block]
            attention_s[zb, rows, :] = attention[:, zb * block : (zb + 1) * block]
        query_flat[:, aligned(h, HEAD_SIZE)] = jnp.dot(
            slopes, keys[...], preferred_element_type=F32
        ).astype(BF16)
        return carry

    lax.fori_loop(0, heads, attend, 0)

    def block_sums(zb, carry):
        sums[zb, 0] = jnp.dot(slopes_s[zb].T, queries[...], preferred_element_type=F32)
        sums[zb, 1] = jnp.dot(attention_s[zb].T, grads[...], preferred_element_type=F32)
        return carry

    lax.fori_loop(0, n_sp, block_sums, 0)

    def sums_copy(side, to, part):
        peer = (z + 1 if side == 0 else z - 1, t)
        return remote(
            leaving.at[to, part],
            arriving.at[side, to, part],
            sums_send.at[to, part],
            sums_recv.at[side, to, part],
            peer,
        )

    def has_upstream(side):
        return z > 0 if side == 0 else z < n_sp - 1

    def sums_wait(side, to, part):
        pltpu.make_async_copy(
            arriving.at[side, to, part],
            arriving.at[side, to, part],
            sums_recv.at[side, to, part],
        ).wait()

    def pass_on(side, far, part):
        to = z + far if side == 0 else z - far
        inside = to < n_sp if side == 0 else to >= 0

        @pl.when(inside)
        def _():
            @pl.when(has_upstream(side))
            def _():
                sums_wait(side, to, part)
                leaving[to, part] = (
                    sums[to, part] + arriving[side, to, part].astype(F32)
                ).astype(BF16)

            @pl.when(jnp.logical_not(has_upstream(side)))
            def _():
                leaving[to, part] = sums[to, part].astype(BF16)

            sums_copy(side, to, part).start()

    def start_edges(side):
        far = n_sp - 1

        for part in range(2):
            pass_on(side, far, part)

    start_edges(0)
    start_edges(1)

    def target_up(j, carry):
        tile = times_transposed(query_flat[...], qw[aligned(j, TILE), :]).astype(BF16)
        for to in range(n_tp):
            up_t[to % 2, to // 2, :, aligned(j, TILE)] = tile[
                to * out_rows : (to + 1) * out_rows
            ]
        return carry

    lax.fori_loop(0, tiles, target_up, 0)

    def pair_copy(which, held, got):
        return remote(
            held.at[1 - core], got, pair_send.at[which], pair_recv.at[which], (z, partner)
        )

    def pair_sum(which, held, got, mid, landed):
        pair_copy(which, held, got).wait_recv()
        for k in list(range(1, n_pair)) + [0]:
            to = across[k - 1] if k else chip
            mid[to] = (held[core, to].astype(F32) + got[to].astype(F32)).astype(BF16)
            if k:
                send(
                    mid.at[to],
                    landed.at[chip],
                    mid_send.at[which, k],
                    mid_recv.at[which, chip],
                    mates[k - 1],
                )

    def last_sum(which, mid, landed):
        total = mid[chip].astype(F32)
        for k in range(1, n_pair):
            came = across[k - 1]
            remote(
                mid.at[came],
                landed.at[came],
                mid_send.at[which, k],
                mid_recv.at[which, came],
                mates[k - 1],
            ).wait_recv()
            total = total + landed[came].astype(F32)
        return total

    target_pair = pair_copy(0, up_t, up_t_pair)
    target_pair.start()
    for far in range(n_sp - 2, 0, -1):
        for part in range(2):
            for side in range(2):
                pass_on(side, far, part)
        if far == n_sp - 2:
            pair_sum(0, up_t, up_t_pair, up_t_mid, up_t_got)
    for part in range(2):
        for side in range(2):

            @pl.when(has_upstream(side))
            def _():
                sums_wait(side, z, part)
                sums[z, part] = sums[z, part] + arriving[side, z, part].astype(F32)

        if part == 0:
            key_all[z] = sums[z, 0].astype(BF16)
            for k in near_first:
                send(
                    key_all.at[z],
                    key_all.at[z],
                    key_send.at[k],
                    key_recv.at[z],
                    others[k - 1],
                )
        else:
            value_flat[...] = sums[z, 1].astype(BF16)

    def source_up(j, carry):
        tile = (
            times_transposed(key_all[z], kw[aligned(j, TILE), :])
            + times_transposed(value_flat[...], vw[aligned(j, TILE), :])
        ).astype(BF16)
        for to in range(n_tp):
            up_s[to % 2, to // 2, :, aligned(j, TILE)] = tile[
                to * src_rows : (to + 1) * src_rows
            ]
        return carry

    lax.fori_loop(0, tiles, source_up, 0)
    source_pair = pair_copy(1, up_s, up_s_pair)
    source_pair.start()

    own = pl.ds(pl.multiple_of(t * out_rows, out_rows), out_rows)
    scaled, inverse = norm_rows(tgt[own, :])
    target_grad[...] = cot[own, :].astype(F32) + norm_back(
        scaled, inverse, target_gain[...], last_sum(0, up_t_mid, up_t_got)
    )
    pair_sum(1, up_s, up_s_pair, up_s_mid, up_s_got)

    def weight_part(step):
        zb = (z + step) % n_sp

        def piece(j, carry):
            product = jnp.dot(
                turned[zb, aligned(j, TILE), :], key_all[zb], preferred_element_type=F32
            )
            if step:
                product = product + key_weight_grad[aligned(j, TILE), :]
            key_weight_grad[aligned(j, TILE), :] = product
            return carry

        lax.fori_loop(0, tiles, piece, 0)

    weight_part(0)
    for k in near_first:
        zb = (z + k) % n_sp
        remote(
            key_all.at[zb], key_all.at[zb], key_send.at[k], key_recv.at[zb], others[k - 1]
        ).wait_recv()
        weight_part(k)

    scaled, inverse = norm_rows(raw[z, t])
    source_grad[...] = norm_back(
        scaled, inverse, source_gain[...], last_sum(1, up_s_mid, up_s_got)
    )
    for copy in pending + [target_pair, source_pair]:
        copy.wait_send()
    for far in range(1, n_sp):
        for part in range(2):
            for side in range(2):
                to = z + far if side == 0 else z - far

                @pl.when(to < n_sp if side == 0 else to >= 0)
                def _():
                    sums_copy(side, to, part).wait_send()


def hand_out(*refs):
    sources, results, held = refs[:3], refs[3:6], refs[6:9]
    in_sem, out_sem = refs[9:]
    reads = [pltpu.make_async_copy(sources[i], held[i], in_sem.at[i]) for i in range(3)]
    writes = [pltpu.make_async_copy(held[i], results[i], out_sem.at[i]) for i in range(3)]
    for read in reads:
        read.start()
    for read, write in zip(reads, writes):
        read.wait()
        write.start()
    for write in writes:
        write.wait()


def on_device_any(
    n_sp,
    n_tp,
    target,
    source,
    cotangent,
    target_gain,
    source_gain,
    query_weight,
    key_weight,
    value_projection_weight,
    output_weight,
):
    tgt_rows, depth = target.shape
    src_rows = source.shape[0]
    out_rows = tgt_rows // n_tp
    if (
        key_weight.shape[1] != HEAD_SIZE
        or n_sp < 2
        or n_tp < 4
        or n_tp % 2
        or depth % TILE
        or tgt_rows % (16 * n_tp)
        or src_rows % 16
        or (src_rows * n_tp) % 128
    ):
        return on_device(
            target,
            source,
            cotangent,
            target_gain,
            source_gain,
            query_weight,
            key_weight,
            value_projection_weight,
            output_weight,
        )
    n_pair = n_tp // 2
    block = src_rows * n_tp
    query_cols = query_weight.shape[1]
    heads = query_cols // HEAD_SIZE
    hbm = pl.BlockSpec(memory_space=pl.ANY)
    vmem = pl.BlockSpec(memory_space=pltpu.VMEM)
    dma = pltpu.SemaphoreType.DMA

    def room(*shape, kind=BF16):
        return pltpu.VMEM(shape, kind)

    results = pl.pallas_call(
        functools.partial(whole_step, n_sp, n_tp),
        out_shape=(
            jax.ShapeDtypeStruct((out_rows, depth), F32),
            jax.ShapeDtypeStruct((src_rows, depth), F32),
            jax.ShapeDtypeStruct((depth, HEAD_SIZE), F32),
        ),
        in_specs=[hbm, hbm, hbm, vmem, vmem, hbm, hbm, hbm, hbm],
        out_specs=(vmem, vmem, vmem),
        scratch_shapes=[
            room(tgt_rows, depth),
            room(tgt_rows, depth),
            room(depth, query_cols),
            room(depth, HEAD_SIZE),
            room(depth, HEAD_SIZE),
            room(query_cols, depth),
            room(n_sp, n_tp, src_rows, depth),
            room(n_sp, block, depth),
            room(n_sp, depth, block),
            room(tgt_rows, depth),
            room(n_sp * block, HEAD_SIZE),
            room(n_sp * block, HEAD_SIZE),
            room(heads * tgt_rows, HEAD_SIZE),
            room(heads * tgt_rows, HEAD_SIZE),
            room(n_sp, heads * tgt_rows, block),
            room(n_sp, heads * tgt_rows, block),
            room(tgt_rows, query_cols),
            room(n_sp, 2, block, HEAD_SIZE, kind=F32),
            room(n_sp, 2, block, HEAD_SIZE),
            room(2, n_sp, 2, block, HEAD_SIZE),
            room(n_sp, block, HEAD_SIZE),
            room(block, HEAD_SIZE),
            room(2, n_pair, out_rows, depth),
            room(n_pair, out_rows, depth),
            room(n_pair, out_rows, depth),
            room(n_pair, out_rows, depth),
            room(2, n_pair, src_rows, depth),
            room(n_pair, src_rows, depth),
            room(n_pair, src_rows, depth),
            room(n_pair, src_rows, depth),
            dma((7,)),
            dma((n_sp, n_tp)),
            dma((n_sp,)),
            dma((n_sp, n_pair)),
            dma((n_sp, n_pair)),
            dma((n_sp, 2)),
            dma((n_sp, 2)),
            dma((n_sp, 2)),
            dma((2, n_sp, 2)),
            dma((n_sp,)),
            dma((n_sp,)),
            dma((2,)),
            dma((2,)),
            dma((2, n_pair)),
            dma((2, n_pair)),
        ],
        compiler_params=pltpu.CompilerParams(
            collective_id=0, has_side_effects=True, vmem_limit_bytes=64 * 1024 * 1024 - 65536
        ),
        name="whole_step",
    )(
        target,
        source,
        cotangent,
        target_gain.reshape(1, depth),
        source_gain.reshape(1, depth),
        query_weight,
        key_weight,
        value_projection_weight,
        output_weight,
    )
    return pl.pallas_call(
        hand_out,
        out_shape=tuple(jax.ShapeDtypeStruct(each.shape, F32) for each in results),
        in_specs=[hbm] * 3,
        out_specs=(hbm,) * 3,
        scratch_shapes=[room(*each.shape, kind=F32) for each in results]
        + [dma((3,)), dma((3,))],
        name="hand_out",
    )(*results)


def solution(mesh):
    return jax.shard_map(
        functools.partial(on_device_any, mesh.shape["sp"], mesh.shape["tp"]),
        mesh=mesh,
        in_specs=(
            P("sp", None),
            P(("sp", "tp"), None),
            P("sp", None),
            P(),
            P(),
            P(None, "tp"),
            P(None, "tp"),
            P(None, "tp"),
            P("tp", None),
        ),
        out_specs=(P(("sp", "tp"), None), P(("sp", "tp"), None), P(None, "tp")),
        check_vma=False,
    )
```

```python
import functools

import jax
import jax.numpy as jnp
from jax import lax
from jax.experimental import pallas as pl
from jax.experimental.pallas import tpu as pltpu
from jax.sharding import PartitionSpec as P

HEAD_SIZE = 256


EPSILON = 1e-05


def as_sent(array):

    def short(part):
        return part.astype(jnp.bfloat16) if part.dtype == jnp.float32 else part

    return jax.tree.map(short, array)


def partner_2(value, axis, bit):
    mask = 2**bit
    pairs = [(source, source ^ mask) for source in range(lax.axis_size(axis))]
    return lax.ppermute(value, axis, pairs)


def combined_all(value, axis, join):
    pieces = jax.tree.map(lambda part: lax.all_gather(part, axis), value)
    head = jax.tree.map(lambda part: part[0], pieces)
    tail = jax.tree.map(lambda part: part[1:], pieces)
    running, _ = lax.scan(lambda running, piece: (join(running, piece), None), head, tail)
    return running


def norm_rows(rows):
    values = rows.astype(jnp.float32)
    centred = values - jnp.mean(values, axis=-1, keepdims=True)
    inverse = lax.rsqrt(jnp.mean(centred * centred, axis=-1, keepdims=True) + EPSILON)
    return (centred * inverse, inverse)


def norm_back(scaled, inverse, gain, upstream):
    weighted = upstream * gain
    spread = jnp.mean(weighted * scaled, axis=-1, keepdims=True)
    return inverse * (weighted - jnp.mean(weighted, axis=-1, keepdims=True) - scaled * spread)


def times_transposed(left, right):
    return lax.dot_general(
        left, right, (((1,), (1,)), ((), ())), preferred_element_type=jnp.float32
    )


def split_heads(flat):
    return flat.reshape(flat.shape[0], flat.shape[1] // HEAD_SIZE, HEAD_SIZE)


def head_scores(queries, key_rows):
    return jnp.einsum(
        "rhd,sd->hrs", queries, key_rows, preferred_element_type=jnp.float32
    ) * HEAD_SIZE ** (-0.5)


def block_statistics(queries, out_grads, key_rows, value_rows):
    scores = head_scores(queries, key_rows)
    highest = jnp.max(scores, axis=2)
    weights = jnp.exp(scores - highest[:, :, None])
    products = jnp.einsum("rhd,sd->hrs", out_grads, value_rows, preferred_element_type=jnp.float32)
    return (highest, jnp.sum(weights, axis=2), jnp.sum(weights * products, axis=2))


def combine_statistics(former, latter):
    highest = jnp.maximum(former[0], latter[0])
    early_scale = jnp.exp(former[0] - highest)
    late_scale = jnp.exp(latter[0] - highest)
    return (
        highest,
        former[1] * early_scale + latter[1] * late_scale,
        former[2] * early_scale + latter[2] * late_scale,
    )


def score_grads(queries, out_grads, key_rows, value_rows, log_total, drifts):
    scores = head_scores(queries, key_rows)
    softmax_weights = jnp.exp(scores - log_total[:, :, None])
    products = jnp.einsum("rhd,sd->hrs", out_grads, value_rows, preferred_element_type=jnp.float32)
    slopes = (softmax_weights * (products - drifts[:, :, None]) * HEAD_SIZE ** (-0.5)).astype(
        jnp.bfloat16
    )
    return (softmax_weights.astype(jnp.bfloat16), slopes)


def join_heads(stacked):
    position = lax.axis_index("tp")
    part_cols = stacked.shape[2]
    bit_level = 0
    while part_cols < HEAD_SIZE:
        partner = jax.tree.map(
            lambda part, own: part.astype(own.dtype),
            partner_2(as_sent(stacked), "tp", bit_level),
            stacked,
        )
        upper_half = position >> bit_level & 1
        stacked = jnp.where(
            upper_half == 0,
            jnp.concatenate((stacked, partner), 2),
            jnp.concatenate((partner, stacked), 2),
        )
        part_cols = part_cols * 2
        bit_level = bit_level + 1
    return stacked


def split_sums(stacked, part_cols):
    position = lax.axis_index("tp")
    bit_count = (HEAD_SIZE // part_cols).bit_length() - 1
    for bit_level in reversed(range(bit_count)):
        half_cols = stacked.shape[2] // 2
        lower_half = stacked[:, :, :half_cols]
        upper_cols = stacked[:, :, half_cols:]
        upper_half = position >> bit_level & 1
        kept_half = jnp.where(upper_half == 0, lower_half, upper_cols)
        sent_half = jnp.where(upper_half == 0, upper_cols, lower_half)
        stacked = kept_half + partner_2(sent_half, "tp", bit_level)
    return stacked


def on_device(
    target,
    source,
    cotangent,
    target_gain,
    source_gain,
    query_weight,
    key_weight,
    value_projection_weight,
    output_weight,
):
    part_cols = key_weight.shape[1]
    src_scaled, src_inverse = norm_rows(source)
    src_normed = (src_scaled * source_gain).astype(jnp.bfloat16)
    tgt_scaled, tgt_inverse = norm_rows(target)
    tgt_normed = (tgt_scaled * target_gain).astype(jnp.bfloat16)
    block_rows = lax.all_gather(src_normed, "tp", axis=0, tiled=True)
    key_portion = jnp.dot(block_rows, key_weight, preferred_element_type=jnp.float32).astype(
        jnp.bfloat16
    )
    value_part = jnp.dot(
        block_rows, value_projection_weight, preferred_element_type=jnp.float32
    ).astype(jnp.bfloat16)
    parted = jnp.stack((key_portion, value_part))
    queries = split_heads(
        jnp.dot(tgt_normed, query_weight, preferred_element_type=jnp.float32).astype(jnp.bfloat16)
    )
    out_grads = split_heads(times_transposed(cotangent, output_weight).astype(jnp.bfloat16))
    head_count = queries.shape[1]
    own_rows = queries.shape[0]
    own_keys = join_heads(parted)
    all_queries, all_grads = (
        lax.all_gather(queries, "sp", axis=0, tiled=True),
        lax.all_gather(out_grads, "sp", axis=0, tiled=True),
    )
    partial_value = block_statistics(all_queries, all_grads, own_keys[0], own_keys[1])
    highest, totals, weighted = combined_all(partial_value, "sp", combine_statistics)
    log_total = highest + jnp.log(totals)
    drifts = weighted / totals
    attention, slopes = score_grads(
        all_queries, all_grads, own_keys[0], own_keys[1], log_total, drifts
    )
    key_gradient_rows = jnp.einsum(
        "hrs,rhd->sd", slopes, all_queries, preferred_element_type=jnp.float32
    )
    value_gradient_rows = jnp.einsum(
        "hrs,rhd->sd", attention, all_grads, preferred_element_type=jnp.float32
    )
    row_start = lax.axis_index("sp") * own_rows
    own_log = lax.dynamic_slice_in_dim(log_total, row_start, own_rows, 1)
    own_drifts = lax.dynamic_slice_in_dim(drifts, row_start, own_rows, 1)
    pieces = lax.all_gather(own_keys, "sp", axis=1, tiled=True)
    unused, slopes = score_grads(queries, out_grads, pieces[0], pieces[1], own_log, own_drifts)
    query_grads = jnp.einsum("hrs,sd->rhd", slopes, pieces[0], preferred_element_type=jnp.float32)
    summed = split_sums(jnp.stack((key_gradient_rows, value_gradient_rows)), part_cols)
    key_flattened = summed[0].astype(jnp.bfloat16)
    value_flattened = summed[1].astype(jnp.bfloat16)
    weight_part = lax.dot_general(
        block_rows, key_flattened, (((0,), (0,)), ((), ())), preferred_element_type=jnp.float32
    )
    key_weight_grad = lax.psum(weight_part.astype(jnp.bfloat16), "sp").astype(jnp.float32)
    source_upstream = lax.psum_scatter(
        (
            times_transposed(key_flattened, key_weight)
            + times_transposed(value_flattened, value_projection_weight)
        ).astype(jnp.bfloat16),
        "tp",
        scatter_dimension=0,
        tiled=True,
    ).astype(jnp.float32)
    source_grad = norm_back(src_scaled, src_inverse, source_gain, source_upstream)
    query_flat = query_grads.astype(jnp.bfloat16).reshape(own_rows, head_count * HEAD_SIZE)
    out_rows = own_rows // lax.axis_size("tp")
    out_start = lax.axis_index("tp") * out_rows
    target_upstream = lax.psum_scatter(
        times_transposed(query_flat, query_weight), "tp", scatter_dimension=0, tiled=True
    )
    slice_scaled = lax.dynamic_slice_in_dim(tgt_scaled, out_start, out_rows, 0)
    slice_inverse = lax.dynamic_slice_in_dim(tgt_inverse, out_start, out_rows, 0)
    slice_cotangent = lax.dynamic_slice_in_dim(cotangent, out_start, out_rows, 0)
    target_grad = slice_cotangent.astype(jnp.float32) + norm_back(
        slice_scaled, slice_inverse, target_gain, target_upstream
    )
    return (target_grad, source_grad, key_weight_grad)


MESH = pl.DeviceIdType.MESH
TILE = 256
BF16 = jnp.bfloat16
F32 = jnp.float32


def aligned(index, size):
    return pl.ds(pl.multiple_of(index * size, size), size)


def whole_step(
    n_sp,
    n_tp,
    target_hbm,
    source_hbm,
    cotangent_hbm,
    target_gain,
    source_gain,
    query_hbm,
    key_hbm,
    value_hbm,
    output_hbm,
    target_grad,
    source_grad,
    key_weight_grad,
    tgt,
    cot,
    qw,
    kw,
    vw,
    ow,
    raw,
    normed,
    turned,
    tgt_normed,
    keys,
    values,
    queries,
    grads,
    slopes_s,
    attention_s,
    query_flat,
    sums,
    leaving,
    arriving,
    key_all,
    value_flat,
    up_t,
    up_t_pair,
    up_t_mid,
    up_t_got,
    up_s,
    up_s_pair,
    up_s_mid,
    up_s_got,
    load_sem,
    gather_sem,
    z_send,
    spread_send,
    forward_send,
    half_send,
    half_recv,
    sums_send,
    sums_recv,
    key_send,
    key_recv,
    pair_send,
    pair_recv,
    mid_send,
    mid_recv,
):
    z = lax.axis_index("sp")
    t = lax.axis_index("tp")
    n_pair = n_tp // 2
    chip = t // 2
    core = t % 2
    partner = chip * 2 + (1 - core)
    depth = tgt.shape[1]
    tgt_rows = tgt.shape[0]
    src_rows = raw.shape[2]
    block = n_tp * src_rows
    out_rows = tgt_rows // n_tp
    heads = qw.shape[1] // HEAD_SIZE
    scale = HEAD_SIZE ** (-0.5)
    tiles = depth // TILE

    def load(index, src, dst):
        return pltpu.make_async_copy(src, dst, load_sem.at[index])

    load_src = load(0, source_hbm, raw.at[z, t])
    load_tgt = load(1, target_hbm, tgt)
    load_qw = load(2, query_hbm, qw)
    load_cot = load(3, cotangent_hbm, cot)
    load_ow = load(4, output_hbm, ow)
    load_kw = load(5, key_hbm, kw)
    load_vw = load(6, value_hbm, vw)
    for each in (load_src, load_tgt, load_qw, load_cot, load_ow, load_kw, load_vw):
        each.start()

    square = n_pair == 4
    if square:
        across = [chip + 1 - 2 * (chip % 2), (chip + 2) % 4, 3 - chip]
    else:
        across = [(chip + k) % n_pair for k in range(1, n_pair)]
    mates = [(z, other * 2 + core) for other in across]
    upper = z // ((n_sp + 1) // 2)
    flipped = z * (1 - 2 * upper) + upper * (n_sp - 1)
    zs = [z]
    for k in range(1, n_sp):
        both = (2 * flipped - k + 2 * n_sp) // (2 * n_sp)
        turn_about = (k + 1) // 2 if k % 2 else -(k // 2)
        place = flipped + both * turn_about + (1 - both) * (k - flipped)
        zs.append(place * (1 - 2 * upper) + upper * (n_sp - 1))
    others = [(zb, t) for zb in zs[1:]]
    barrier = pltpu.get_barrier_semaphore()
    for peer in mates + others + [(z, partner)]:
        pl.semaphore_signal(barrier, inc=1, device_id=peer, device_id_type=MESH)
    pl.semaphore_wait(barrier, len(mates) + len(others) + 1)

    def remote(src, dst, send, recv, peer):
        return pltpu.make_async_remote_copy(
            src_ref=src,
            dst_ref=dst,
            send_sem=send,
            recv_sem=recv,
            device_id=peer,
            device_id_type=MESH,
        )

    pending = []

    def send(*args):
        copy = remote(*args)
        copy.start()
        pending.append(copy)

    def row_copy(zb, tb, sem, peer):
        return (raw.at[zb, tb], raw.at[zb, tb], sem, gather_sem.at[zb, tb], peer)

    def arrive(zb, tb):
        remote(*row_copy(zb, tb, z_send.at[0], (z, partner))).wait_recv()

    def spread(step):
        zb = zs[step]
        if step:
            arrive(zb, t)
        for k in range(1, n_pair):
            if not square or k != 3:
                send(*row_copy(zb, t, spread_send.at[step, k], mates[k - 1]))
        send(*row_copy(zb, t, spread_send.at[step, 0], (z, partner)))

    def forward(step):
        zb = zs[step]
        for k in range(1, n_pair):
            tb = mates[k - 1][1]
            if square and k == 3:
                continue
            arrive(zb, tb)
            if square:
                send(*half_copy(zb, tb, k - 1, half_send.at[step, k - 1], mates[2 - k]))
            send(*row_copy(zb, tb, forward_send.at[step, k], (z, partner)))

    def half_copy(zb, tb, half, sem, peer):
        part = raw.at[zb, tb, pl.ds(half * (src_rows // 2), src_rows // 2)]
        return (part, part, sem, half_recv.at[zb, half], peer)

    def far_corner(step):
        if not square:
            return
        zb = zs[step]
        tb = mates[2][1]
        for half in range(2):
            remote(*half_copy(zb, tb, half, half_send.at[step, half], mates[0])).wait_recv()
        send(*row_copy(zb, tb, forward_send.at[step, 3], (z, partner)))

    def source_block(step):
        zb = zs[step]
        for other in [chip] + across:
            arrive(zb, other * 2 + 1 - core)
        gain = source_gain[...]

        def norm_piece(piece, carry):
            scaled, _ = norm_rows(raw[zb, piece])
            normed[zb, aligned(piece, src_rows), :] = (scaled * gain).astype(BF16)
            return carry

        lax.fori_loop(0, n_tp, norm_piece, 0)
        keys[aligned(zb, block), :] = jnp.dot(
            normed[zb], kw[...], preferred_element_type=F32
        ).astype(BF16)
        values[aligned(zb, block), :] = jnp.dot(
            normed[zb], vw[...], preferred_element_type=F32
        ).astype(BF16)

        def turn(j, carry):
            turned[zb, aligned(j, TILE), :] = normed[zb, :, aligned(j, TILE)].T
            return carry

        lax.fori_loop(0, tiles, turn, 0)

    near_first = range(1, n_sp)
    load_src.wait()
    for k in near_first:
        send(*row_copy(z, t, z_send.at[k], others[k - 1]))
    spread(0)

    load_tgt.wait()
    norm_step = tgt_rows // n_tp

    def norm_target(piece, carry):
        scaled, _ = norm_rows(tgt[aligned(piece, norm_step), :])
        tgt_normed[aligned(piece, norm_step), :] = (scaled * target_gain[...]).astype(BF16)
        return carry

    lax.fori_loop(0, n_tp, norm_target, 0)
    load_qw.wait()

    def query_head(h, carry):
        queries[aligned(h, tgt_rows), :] = jnp.dot(
            tgt_normed[...], qw[:, aligned(h, HEAD_SIZE)], preferred_element_type=F32
        ).astype(BF16)
        return carry

    lax.fori_loop(0, heads, query_head, 0)
    forward(0)
    spread(1)
    load_cot.wait()
    load_ow.wait()

    def grad_head(h, carry):
        grads[aligned(h, tgt_rows), :] = times_transposed(
            cot[...], ow[aligned(h, HEAD_SIZE), :]
        ).astype(BF16)
        return carry

    lax.fori_loop(0, heads, grad_head, 0)
    load_kw.wait()
    load_vw.wait()
    for step in range(n_sp):
        far_corner(step)
        if step + 1 < n_sp:
            forward(step + 1)
        if step + 2 < n_sp:
            spread(step + 2)
        source_block(step)

    def attend(h, carry):
        rows = aligned(h, tgt_rows)
        scores = times_transposed(queries[rows, :], keys[...]) * scale
        highest = jnp.max(scores, axis=1, keepdims=True)
        weights = jnp.exp(scores - highest)
        totals = jnp.sum(weights, axis=1, keepdims=True)
        products = times_transposed(grads[rows, :], values[...])
        drifts = jnp.sum(weights * products, axis=1, keepdims=True) / totals
        weights = weights * (1.0 / totals)
        attention = weights.astype(BF16)
        slopes = (weights * (products - drifts) * scale).astype(BF16)
        for zb in range(n_sp):
            slopes_s[zb, rows, :] = slopes[:, zb * block : (zb + 1) * block]
            attention_s[zb, rows, :] = attention[:, zb * block : (zb + 1) * block]
        query_flat[:, aligned(h, HEAD_SIZE)] = jnp.dot(
            slopes, keys[...], preferred_element_type=F32
        ).astype(BF16)
        return carry

    lax.fori_loop(0, heads, attend, 0)

    def block_sums(zb, carry):
        sums[zb, 0] = jnp.dot(slopes_s[zb].T, queries[...], preferred_element_type=F32)
        sums[zb, 1] = jnp.dot(attention_s[zb].T, grads[...], preferred_element_type=F32)
        return carry

    lax.fori_loop(0, n_sp, block_sums, 0)

    def sums_copy(side, to, part):
        peer = (z + 1 if side == 0 else z - 1, t)
        return remote(
            leaving.at[to, part],
            arriving.at[side, to, part],
            sums_send.at[to, part],
            sums_recv.at[side, to, part],
            peer,
        )

    def has_upstream(side):
        return z > 0 if side == 0 else z < n_sp - 1

    def sums_wait(side, to, part):
        pltpu.make_async_copy(
            arriving.at[side, to, part],
            arriving.at[side, to, part],
            sums_recv.at[side, to, part],
        ).wait()

    def pass_on(side, far, part):
        to = z + far if side == 0 else z - far
        inside = to < n_sp if side == 0 else to >= 0

        @pl.when(inside)
        def _():
            @pl.when(has_upstream(side))
            def _():
                sums_wait(side, to, part)
                leaving[to, part] = (
                    sums[to, part] + arriving[side, to, part].astype(F32)
                ).astype(BF16)

            @pl.when(jnp.logical_not(has_upstream(side)))
            def _():
                leaving[to, part] = sums[to, part].astype(BF16)

            sums_copy(side, to, part).start()

    def start_edges(side):
        far = n_sp - 1

        for part in range(2):
            pass_on(side, far, part)

    start_edges(0)
    start_edges(1)

    def target_up(j, carry):
        tile = times_transposed(query_flat[...], qw[aligned(j, TILE), :]).astype(BF16)
        for to in range(n_tp):
            up_t[to % 2, to // 2, :, aligned(j, TILE)] = tile[
                to * out_rows : (to + 1) * out_rows
            ]
        return carry

    lax.fori_loop(0, tiles, target_up, 0)

    def pair_copy(which, held, got):
        return remote(
            held.at[1 - core], got, pair_send.at[which], pair_recv.at[which], (z, partner)
        )

    def pair_sum(which, held, got, mid, landed):
        pair_copy(which, held, got).wait_recv()
        for k in list(range(1, n_pair)) + [0]:
            to = across[k - 1] if k else chip
            mid[to] = (held[core, to].astype(F32) + got[to].astype(F32)).astype(BF16)
            if k:
                send(
                    mid.at[to],
                    landed.at[chip],
                    mid_send.at[which, k],
                    mid_recv.at[which, chip],
                    mates[k - 1],
                )

    def last_sum(which, mid, landed):
        total = mid[chip].astype(F32)
        for k in range(1, n_pair):
            came = across[k - 1]
            remote(
                mid.at[came],
                landed.at[came],
                mid_send.at[which, k],
                mid_recv.at[which, came],
                mates[k - 1],
            ).wait_recv()
            total = total + landed[came].astype(F32)
        return total

    target_pair = pair_copy(0, up_t, up_t_pair)
    target_pair.start()
    for far in range(n_sp - 2, 0, -1):
        for part in range(2):
            for side in range(2):
                pass_on(side, far, part)
        if far == n_sp - 2:
            pair_sum(0, up_t, up_t_pair, up_t_mid, up_t_got)
    for part in range(2):
        for side in range(2):

            @pl.when(has_upstream(side))
            def _():
                sums_wait(side, z, part)
                sums[z, part] = sums[z, part] + arriving[side, z, part].astype(F32)

        if part == 0:
            key_all[z] = sums[z, 0].astype(BF16)
            for k in near_first:
                send(
                    key_all.at[z],
                    key_all.at[z],
                    key_send.at[k],
                    key_recv.at[z],
                    others[k - 1],
                )
        else:
            value_flat[...] = sums[z, 1].astype(BF16)

    def source_up(j, carry):
        tile = (
            times_transposed(key_all[z], kw[aligned(j, TILE), :])
            + times_transposed(value_flat[...], vw[aligned(j, TILE), :])
        ).astype(BF16)
        for to in range(n_tp):
            up_s[to % 2, to // 2, :, aligned(j, TILE)] = tile[
                to * src_rows : (to + 1) * src_rows
            ]
        return carry

    lax.fori_loop(0, tiles, source_up, 0)
    source_pair = pair_copy(1, up_s, up_s_pair)
    source_pair.start()

    own = pl.ds(pl.multiple_of(t * out_rows, out_rows), out_rows)
    scaled, inverse = norm_rows(tgt[own, :])
    target_grad[...] = cot[own, :].astype(F32) + norm_back(
        scaled, inverse, target_gain[...], last_sum(0, up_t_mid, up_t_got)
    )
    pair_sum(1, up_s, up_s_pair, up_s_mid, up_s_got)

    def weight_part(step):
        zb = zs[step]

        def piece(j, carry):
            product = jnp.dot(
                turned[zb, aligned(j, TILE), :], key_all[zb], preferred_element_type=F32
            )
            if step:
                product = product + key_weight_grad[aligned(j, TILE), :]
            key_weight_grad[aligned(j, TILE), :] = product
            return carry

        lax.fori_loop(0, tiles, piece, 0)

    weight_part(0)
    for k in near_first:
        zb = zs[k]
        remote(
            key_all.at[zb], key_all.at[zb], key_send.at[k], key_recv.at[zb], others[k - 1]
        ).wait_recv()
        weight_part(k)

    scaled, inverse = norm_rows(raw[z, t])
    source_grad[...] = norm_back(
        scaled, inverse, source_gain[...], last_sum(1, up_s_mid, up_s_got)
    )
    for copy in pending + [target_pair, source_pair]:
        copy.wait_send()
    for far in range(1, n_sp):
        for part in range(2):
            for side in range(2):
                to = z + far if side == 0 else z - far

                @pl.when(to < n_sp if side == 0 else to >= 0)
                def _():
                    sums_copy(side, to, part).wait_send()


def hand_out(*refs):
    sources, results, held = refs[:3], refs[3:6], refs[6:9]
    in_sem, out_sem = refs[9:]
    reads = [pltpu.make_async_copy(sources[i], held[i], in_sem.at[i]) for i in range(3)]
    writes = [pltpu.make_async_copy(held[i], results[i], out_sem.at[i]) for i in range(3)]
    for read in reads:
        read.start()
    for read, write in zip(reads, writes):
        read.wait()
        write.start()
    for write in writes:
        write.wait()


def on_device_any(
    n_sp,
    n_tp,
    target,
    source,
    cotangent,
    target_gain,
    source_gain,
    query_weight,
    key_weight,
    value_projection_weight,
    output_weight,
):
    tgt_rows, depth = target.shape
    src_rows = source.shape[0]
    out_rows = tgt_rows // n_tp
    if (
        key_weight.shape[1] != HEAD_SIZE
        or n_sp < 2
        or n_tp < 4
        or n_tp % 2
        or depth % TILE
        or tgt_rows % (16 * n_tp)
        or src_rows % 16
        or (src_rows * n_tp) % 128
    ):
        return on_device(
            target,
            source,
            cotangent,
            target_gain,
            source_gain,
            query_weight,
            key_weight,
            value_projection_weight,
            output_weight,
        )
    n_pair = n_tp // 2
    block = src_rows * n_tp
    query_cols = query_weight.shape[1]
    heads = query_cols // HEAD_SIZE
    hbm = pl.BlockSpec(memory_space=pl.ANY)
    vmem = pl.BlockSpec(memory_space=pltpu.VMEM)
    dma = pltpu.SemaphoreType.DMA

    def room(*shape, kind=BF16):
        return pltpu.VMEM(shape, kind)

    results = pl.pallas_call(
        functools.partial(whole_step, n_sp, n_tp),
        out_shape=(
            jax.ShapeDtypeStruct((out_rows, depth), F32),
            jax.ShapeDtypeStruct((src_rows, depth), F32),
            jax.ShapeDtypeStruct((depth, HEAD_SIZE), F32),
        ),
        in_specs=[hbm, hbm, hbm, vmem, vmem, hbm, hbm, hbm, hbm],
        out_specs=(vmem, vmem, vmem),
        scratch_shapes=[
            room(tgt_rows, depth),
            room(tgt_rows, depth),
            room(depth, query_cols),
            room(depth, HEAD_SIZE),
            room(depth, HEAD_SIZE),
            room(query_cols, depth),
            room(n_sp, n_tp, src_rows, depth),
            room(n_sp, block, depth),
            room(n_sp, depth, block),
            room(tgt_rows, depth),
            room(n_sp * block, HEAD_SIZE),
            room(n_sp * block, HEAD_SIZE),
            room(heads * tgt_rows, HEAD_SIZE),
            room(heads * tgt_rows, HEAD_SIZE),
            room(n_sp, heads * tgt_rows, block),
            room(n_sp, heads * tgt_rows, block),
            room(tgt_rows, query_cols),
            room(n_sp, 2, block, HEAD_SIZE, kind=F32),
            room(n_sp, 2, block, HEAD_SIZE),
            room(2, n_sp, 2, block, HEAD_SIZE),
            room(n_sp, block, HEAD_SIZE),
            room(block, HEAD_SIZE),
            room(2, n_pair, out_rows, depth),
            room(n_pair, out_rows, depth),
            room(n_pair, out_rows, depth),
            room(n_pair, out_rows, depth),
            room(2, n_pair, src_rows, depth),
            room(n_pair, src_rows, depth),
            room(n_pair, src_rows, depth),
            room(n_pair, src_rows, depth),
            dma((7,)),
            dma((n_sp, n_tp)),
            dma((n_sp,)),
            dma((n_sp, n_pair)),
            dma((n_sp, n_pair)),
            dma((n_sp, 2)),
            dma((n_sp, 2)),
            dma((n_sp, 2)),
            dma((2, n_sp, 2)),
            dma((n_sp,)),
            dma((n_sp,)),
            dma((2,)),
            dma((2,)),
            dma((2, n_pair)),
            dma((2, n_pair)),
        ],
        compiler_params=pltpu.CompilerParams(
            collective_id=0, has_side_effects=True, vmem_limit_bytes=64 * 1024 * 1024 - 65536
        ),
        name="whole_step",
    )(
        target,
        source,
        cotangent,
        target_gain.reshape(1, depth),
        source_gain.reshape(1, depth),
        query_weight,
        key_weight,
        value_projection_weight,
        output_weight,
    )
    return pl.pallas_call(
        hand_out,
        out_shape=tuple(jax.ShapeDtypeStruct(each.shape, F32) for each in results),
        in_specs=[hbm] * 3,
        out_specs=(hbm,) * 3,
        scratch_shapes=[room(*each.shape, kind=F32) for each in results]
        + [dma((3,)), dma((3,))],
        name="hand_out",
    )(*results)


def solution(mesh):
    return jax.shard_map(
        functools.partial(on_device_any, mesh.shape["sp"], mesh.shape["tp"]),
        mesh=mesh,
        in_specs=(
            P("sp", None),
            P(("sp", "tp"), None),
            P("sp", None),
            P(),
            P(),
            P(None, "tp"),
            P(None, "tp"),
            P(None, "tp"),
            P("tp", None),
        ),
        out_specs=(P(("sp", "tp"), None), P(("sp", "tp"), None), P(None, "tp")),
        check_vma=False,
    )
```
